32 devices in a mesh: sp: 8 (over z, x), tp: 4 (over y, core).
Axes of the slice: x: 2, y: 2, z: 4, core: 2. Of those that a mesh axis runs over, the one named last changes fastest.
Arguments:
- out_cotangent: bfloat16 [2048, 2048], P('sp'), may hold values from -6 to 6
- stream: bfloat16 [2048, 2048], P('sp'), may hold values from -6 to 6
- route_ids: int32 [2048, 2], P('sp'), may hold values from 0 to 7, all different within a row; in each aligned block of 256 rows (0 to 255, 256 to 511, ...) at most 128 rows name the same one
- route_weights: float32 [2048, 2], P('sp'), may hold values from 0.3 to 2
- gate_proj: bfloat16 [8, 2048, 1024], P('sp', None, 'tp'), may hold values from -0.125 to 0.125
- up_proj: bfloat16 [8, 2048, 1024], P('sp', None, 'tp'), may hold values from -0.125 to 0.125
- down_proj: bfloat16 [8, 1024, 2048], P('sp', 'tp'), may hold values from -0.1875 to 0.1875
- outer_gate: bfloat16 [2048, 512], P('sp', 'tp'), may hold values from -6 to 6
- inner_gate: bfloat16 [2048, 512], P('sp', 'tp'), may hold values from -6 to 6
- conv_input: bfloat16 [2048, 512], P('sp', 'tp'), may hold values from -6 to 6
- conv_taps: float32 [3, 512], P(None, 'tp'), may hold values from -4 to 4
- out_proj: bfloat16 [2048, 512], P(None, 'tp'), may hold values from -0.25 to 0.25
Outputs:
- grad_gate_proj: bfloat16 [8, 2048, 1024], P('sp', None, 'tp')
- grad_up_proj: bfloat16 [8, 2048, 1024], P('sp', None, 'tp')
- grad_down_proj: bfloat16 [8, 1024, 2048], P('sp', 'tp')
- grad_out_proj: float32 [2048, 512], P('sp', 'tp')
- grad_outer_gate: float32 [2048, 512], P('sp', 'tp')
- grad_inner_gate: float32 [2048, 512], P('sp', 'tp')
- grad_conv_input: float32 [2048, 512], P('sp', 'tp')
The draws below stay inside these ranges and needn't reach their ends.
Inputs may be any that keep to these rules, and one draw needn't show every extreme that they name: `route_ids`: the 2 experts of a token differ. Among the tokens of one index of sp, no expert is chosen more than 128 times, and in every draw some expert is chosen exactly 128 times by them.
All inputs are finite; a program needn't handle non-finite values.
Results may differ from the reference program's by a relative error of at most 0.018.
Values may be sent and summed in bfloat16 or wider, within the bound.
A program may use at most 64 MiB of HBM per device.

```python
import math
import jax
import jax.numpy as jnp
import numpy as np
from jax import lax

D = 2048
FF = 1024
CONV = 512
TAPS = 3
TOPK = 2
TOK_DEV = 256
EXPERTS = 8
CAP = 128
SLOTS = 1024
TOKENS = 2048
N_TP = 4


def with_spikes(entries, rng, source, target, shards_of, factor):
    owner, partner = [(jnp.arange(entries.shape[dim]) // (entries.shape[dim] // shards_of)).reshape([-1 if axis == dim else 1 for axis in range(entries.ndim)]) for dim in (source, target)]
    chosen = jax.random.permutation(rng, shards_of)[partner]
    strong = (owner == chosen) | (owner == (partner + shards_of // 2) % shards_of)
    return jnp.where(strong, factor * entries, entries)


def block_levels(stream_key, dims, cuts, low, largest):
    def one(dim, parts):
        heights = jax.random.uniform(jax.random.fold_in(jax.random.fold_in(stream_key, 6), dim), (parts,), jnp.float32, low / len(cuts), largest / len(cuts))
        return jnp.repeat(jnp.exp(heights), dims[dim] // parts).reshape((-1,) + (1,) * (len(dims) - dim - 1))

    gain = one(*cuts[0])
    for cut in cuts[1:]:
        gain = gain * one(*cut)
    return gain


def deal_out(own_key, own, number, rows, count, top, reach, lean):
    sequence = jax.random.permutation(own_key, count)
    heavy_load, ordinary = shares(count, rows * top, reach, lean, True), shares(count, rows * top, reach, lean, False)
    places = jnp.arange(count)

    def named(tallies, turn):
        used = int((tallies > 0).sum())
        fixed = max(1, used // 4)
        moved = fixed + (places - fixed + turn * (used - fixed)) % max(1, count - fixed)
        return jnp.zeros((count,), jnp.int32).at[sequence[jnp.where(places < fixed, places, moved)]].set(jnp.asarray(tallies, jnp.int32))

    tallies = jnp.where(number % 4 == 0, named(heavy_load, number // 4), named(ordinary, number - number // 4 - 1))
    mixed = jax.random.permutation(jax.random.fold_in(own, 3), count)
    donor, sink = mixed[0:count // 2 * 2:2], mixed[1:count // 2 * 2:2]
    room = jnp.minimum(tallies[donor] - 1, reach - tallies[sink]) // 2
    room = jnp.where((donor == sequence[0]) | (sink == sequence[0]) | (tallies[sink] == 0), 0, jnp.maximum(room, 0))
    moved = jax.random.randint(jax.random.fold_in(own, 4), (count // 2,), 0, 1 << 20) % (room + 1)
    tallies = tallies.at[donor].add(-moved).at[sink].add(moved)
    labels = jnp.searchsorted(jnp.cumsum(tallies), jnp.arange(rows * top), side="right").astype(jnp.int32)
    table = labels.reshape(top, rows).T
    table = table[jax.random.permutation(jax.random.fold_in(own, 1), rows)]
    turn = jax.random.randint(jax.random.fold_in(own, 2), (rows, 1), 0, top)
    return jnp.take_along_axis(table, (jnp.arange(top)[None, :] + turn) % top, axis=1)


def shares(number_of, total, reach, skew, full):
    portions = [(1 << 20) // math.isqrt(grade ** skew) + 1 for grade in range(1, number_of + 1)]
    largest = reach if full else min(reach, max(-(-total // number_of), total * portions[0] // sum(portions)))
    least = 1 if total - largest >= number_of - 1 else 0
    counts, rest = [largest] + [least] * (number_of - 1), total - largest - least * (number_of - 1)
    while rest > 0:
        movable = [i for i in range(1, number_of) if counts[i] < largest] or [i for i in range(1, number_of) if counts[i] < reach]
        whole, left = sum([portions[i] for i in movable]), rest
        for i in movable:
            more = min(reach - counts[i], max(1, left * portions[i] // whole), rest)
            counts[i] = counts[i] + more
            rest = rest - more
    return np.array(counts)


def bell_draw(own_key, dims, deviation, bound, cuts=(), kind=jnp.bfloat16):
    loudness = block_levels(own_key, dims, cuts, -0.22, 0.18) if cuts else 1.0
    entries = jax.random.normal(own_key, dims, jnp.float32) * deviation * loudness
    return jnp.minimum(jnp.maximum(entries, -bound), bound).astype(kind)


def bell_draw_with(stream_key, extent, width, most, cuts, heavy, kind=jnp.bfloat16):
    values = width * jax.random.normal(stream_key, extent, jnp.float32)
    if cuts:
        values = values * block_levels(stream_key, extent, cuts, -0.22, 0.18)
    return jnp.clip(with_spikes(values, jax.random.fold_in(stream_key, 3), *heavy), -most, most).astype(kind)


def setup_inputs(seed: int = 0) -> dict:
    seeds = jax.random.split(jax.random.key(seed), 13)
    out_cotangent = bell_draw_with(seeds[0], (TOKENS, D), 1.0, 6.0, ((0, 8),), (0, 1, 8, 2.0))
    stream = bell_draw(seeds[1], (TOKENS, D), 1.0, 6.0, ((0, 8),))
    route_ids_keys = jax.random.split(jax.random.fold_in(seeds[2], 1), TOKENS // TOK_DEV)
    route_ids_turns = jax.random.permutation(jax.random.fold_in(seeds[2], 3), TOKENS // TOK_DEV)
    route_ids = jax.vmap(lambda own, number: deal_out(jax.random.fold_in(seeds[2], 2), own, number, TOK_DEV, EXPERTS, TOPK, CAP, 1))(route_ids_keys, route_ids_turns).reshape((TOKENS, TOPK))
    route_weights = jnp.clip(0.3 + 1.7 * jax.random.uniform(seeds[3], (TOKENS, TOPK), jnp.float32) ** block_levels(seeds[3], (TOKENS, TOPK), ((0, 8),), -0.2, 0.2), 0.3, 2.0)
    gate_proj = bell_draw(seeds[4], (EXPERTS, D, FF), D ** -0.5, 0.125, ((0, 8), (2, 4)))
    up_proj = bell_draw(seeds[5], (EXPERTS, D, FF), D ** -0.5, 0.125, ((0, 8), (2, 4)))
    down_proj = bell_draw(seeds[6], (EXPERTS, FF, D), FF ** -0.5, 0.1875, ((0, 8), (1, 4)))
    outer_gate = bell_draw(seeds[7], (TOKENS, CONV), 1.0, 6.0, ((0, 8), (1, 4)))
    inner_gate = bell_draw(seeds[8], (TOKENS, CONV), 1.0, 6.0, ((0, 8), (1, 4)))
    conv_input = bell_draw(seeds[9], (TOKENS, CONV), 1.0, 6.0, ((0, 8), (1, 4)))
    conv_taps = bell_draw(seeds[10], (TAPS, CONV), 0.6, 4.0, ((1, 4),), jnp.float32)
    out_proj = bell_draw(seeds[11], (D, CONV), CONV ** -0.5, 0.25, ((1, 4),))
    return dict(out_cotangent=out_cotangent, stream=stream, route_ids=route_ids, route_weights=route_weights, gate_proj=gate_proj, up_proj=up_proj, down_proj=down_proj, outer_gate=outer_gate, inner_gate=inner_gate, conv_input=conv_input, conv_taps=conv_taps, out_proj=out_proj)


def expert_backward(out_cotangent, stream, route_ids, route_weights, w_gate, w_up, w_down, expert):
    chosen = route_ids == expert
    weight = jnp.sum(jnp.where(chosen, route_weights, 0.0), axis=1)
    hit = jnp.any(chosen, axis=1)
    index = jnp.nonzero(hit, size=SLOTS, fill_value=0)[0].astype(jnp.int32)
    count = jnp.sum(hit.astype(jnp.int32))
    valid = jnp.arange(SLOTS, dtype=jnp.int32) < count
    rows_input = jnp.where(valid[:, None], stream[index], jnp.zeros((), jnp.bfloat16))
    rows_grad = (weight[index][:, None] * out_cotangent[index].astype(jnp.float32))
    rows_grad = jnp.where(valid[:, None], rows_grad, 0.0).astype(jnp.bfloat16)
    gate = jnp.dot(rows_input, w_gate, preferred_element_type=jnp.float32)
    up = jnp.dot(rows_input, w_up, preferred_element_type=jnp.float32)
    sig = jax.nn.sigmoid(gate)
    silu_gate = gate * sig
    hidden = (silu_gate * up).astype(jnp.bfloat16)
    d_hidden = lax.dot_general(rows_grad, w_down, (((1,), (1,)), ((), ())), preferred_element_type=jnp.float32)
    d_gate = (d_hidden * up * sig * (1.0 + gate * (1.0 - sig))).astype(jnp.bfloat16)
    d_up = (d_hidden * silu_gate).astype(jnp.bfloat16)
    over_rows = (((0,), (0,)), ((), ()))
    grad_down = lax.dot_general(hidden, rows_grad, over_rows, preferred_element_type=jnp.float32).astype(jnp.bfloat16)
    grad_gate = lax.dot_general(rows_input, d_gate, over_rows, preferred_element_type=jnp.float32).astype(jnp.bfloat16)
    grad_up = lax.dot_general(rows_input, d_up, over_rows, preferred_element_type=jnp.float32).astype(jnp.bfloat16)
    block = FF // N_TP
    gate_blocks = d_gate.astype(jnp.float32).reshape(SLOTS, N_TP, block)
    up_blocks = d_up.astype(jnp.float32).reshape(SLOTS, N_TP, block)
    wg_blocks = w_gate.astype(jnp.float32).reshape(D, N_TP, block)
    wu_blocks = w_up.astype(jnp.float32).reshape(D, N_TP, block)
    partials = jnp.einsum('snf,dnf->nsd', gate_blocks, wg_blocks) + jnp.einsum('snf,dnf->nsd', up_blocks, wu_blocks)
    partials = partials.astype(jnp.bfloat16).astype(jnp.float32)
    row_grad = jnp.sum(partials, axis=0).astype(jnp.bfloat16)
    row_grad = jnp.where(valid[:, None], row_grad.astype(jnp.float32), 0.0)
    return index, row_grad, grad_gate, grad_up, grad_down


def reference(out_cotangent, stream, route_ids, route_weights, gate_proj, up_proj, down_proj,
              outer_gate, inner_gate, conv_input, conv_taps, out_proj):
    def step(carry, inputs):
        w_gate, w_up, w_down, expert = inputs
        index, row_grad, grad_gate, grad_up, grad_down = expert_backward(
            out_cotangent, stream, route_ids, route_weights, w_gate, w_up, w_down, expert)
        carry = carry.at[index].add(row_grad)
        return carry, (grad_gate, grad_up, grad_down)

    moe_grad, grads = lax.scan(step, jnp.zeros((TOKENS, D), jnp.float32),
                               (gate_proj, up_proj, down_proj, jnp.arange(EXPERTS, dtype=jnp.int32)))
    grad_gate_proj, grad_up_proj, grad_down_proj = grads
    stream_grad = (out_cotangent.astype(jnp.float32) + moe_grad).astype(jnp.bfloat16)
    mixed = inner_gate.astype(jnp.float32) * conv_input.astype(jnp.float32)
    padded = jnp.concatenate([jnp.zeros((2, CONV), jnp.float32), mixed], axis=0)
    conv_out = conv_taps[0] * padded[:TOKENS] + conv_taps[1] * padded[1:TOKENS + 1] + conv_taps[2] * padded[2:]
    mixer_out = (outer_gate.astype(jnp.float32) * conv_out).astype(jnp.bfloat16)
    d_mixer = jnp.dot(stream_grad, out_proj, preferred_element_type=jnp.float32)
    grad_outer_gate = d_mixer * conv_out
    d_conv = d_mixer * outer_gate.astype(jnp.float32)
    trailing = jnp.concatenate([d_conv, jnp.zeros((2, CONV), jnp.float32)], axis=0)
    d_mixed = conv_taps[2] * trailing[:TOKENS] + conv_taps[1] * trailing[1:TOKENS + 1] + conv_taps[0] * trailing[2:]
    grad_inner_gate = d_mixed * conv_input.astype(jnp.float32)
    grad_conv_input = d_mixed * inner_gate.astype(jnp.float32)
    grad_out_proj = lax.dot_general(stream_grad, mixer_out, (((0,), (0,)), ((), ())), preferred_element_type=jnp.float32)
    return (grad_gate_proj, grad_up_proj, grad_down_proj, grad_out_proj,
            grad_outer_gate, grad_inner_gate, grad_conv_input)
```

```python
import jax
import jax.numpy as jnp
from jax import lax
from jax.sharding import PartitionSpec as P


def passed_along(x, axis, by):
    devices = lax.axis_size(axis)
    pairs = [(i, i + by) for i in range(devices) if 0 <= i + by < devices]
    return lax.ppermute(x, axis, pairs)


def to_owners(x, devices):
    blocks = x.reshape(devices, -1, x.shape[1])
    return lax.all_to_all(blocks, "sp", split_axis=0, concat_axis=0, tiled=True).reshape(x.shape)


def shards(
    out_cotangent,
    stream,
    route_ids,
    route_weights,
    gate_proj,
    up_proj,
    down_proj,
    outer_gate,
    inner_gate,
    conv_input,
    conv_taps,
    out_proj,
):
    sp_devices = lax.axis_size("sp")
    tokens_here, width = stream.shape
    experts = sp_devices * gate_proj.shape[0]
    capacity = 4 * tokens_here // experts
    quarter = width // lax.axis_size("tp")
    first_column = lax.axis_index("tp") * quarter
    own_cotangent = lax.dynamic_slice_in_dim(out_cotangent, first_column, quarter, 1)
    own_stream = lax.dynamic_slice_in_dim(stream, first_column, quarter, 1)
    over_rows = (((0,), (0,)), ((), ()))
    expert_ids = jnp.arange(experts, dtype=jnp.int32)
    chosen = route_ids[:, :, None] == expert_ids
    hit = jnp.any(chosen, axis=1)
    token_weight = jnp.sum(jnp.where(chosen, route_weights[:, :, None], 0.0), axis=1)
    token_ids = jnp.arange(tokens_here, dtype=jnp.int32)
    below = (token_ids[:, None] < token_ids[None, :]).astype(jnp.bfloat16)
    rank = lax.dot_general(
        hit.astype(jnp.bfloat16), below, over_rows, preferred_element_type=jnp.float32
    )
    rank = jnp.where(hit.T, rank, -1.0)
    in_slot = rank[:, None, :] == jnp.arange(capacity, dtype=jnp.float32)[None, :, None]
    slot_weight = jnp.sum(jnp.where(in_slot, token_weight.T[:, None, :], 0.0), axis=2)
    pick = in_slot.astype(jnp.bfloat16).reshape(experts * capacity, tokens_here)
    send_input = jnp.dot(pick, own_stream, preferred_element_type=jnp.float32).astype(jnp.bfloat16)
    send_grad = (
        slot_weight.reshape(-1, 1)
        * jnp.dot(pick, own_cotangent, preferred_element_type=jnp.float32)
    ).astype(jnp.bfloat16)
    got_input = to_owners(send_input, sp_devices)
    rows_input = lax.all_gather(got_input, "tp", axis=1, tiled=True)
    send_grad, got_input = lax.optimization_barrier((send_grad, got_input))
    got_grad = to_owners(send_grad, sp_devices)
    rows_grad = lax.all_gather(got_grad, "tp", axis=1, tiled=True)
    mixed = inner_gate.astype(jnp.float32) * conv_input.astype(jnp.float32)
    previous = passed_along(mixed[tokens_here - 2 :], "sp", 1)
    extended = jnp.concatenate([previous, mixed], axis=0)
    conv_out = (
        conv_taps[0] * extended[:tokens_here]
        + conv_taps[1] * extended[1 : tokens_here + 1]
        + conv_taps[2] * extended[2:]
    )
    mixer_out = (outer_gate.astype(jnp.float32) * conv_out).astype(jnp.bfloat16)
    conv_out, mixer_out, rows_grad = lax.optimization_barrier((conv_out, mixer_out, rows_grad))
    w_gate = gate_proj[0]
    w_up = up_proj[0]
    w_down = down_proj[0]
    gate = jnp.dot(rows_input, w_gate, preferred_element_type=jnp.float32)
    up = jnp.dot(rows_input, w_up, preferred_element_type=jnp.float32)
    sig = jax.nn.sigmoid(gate)
    silu_gate = gate * sig
    hidden = (silu_gate * up).astype(jnp.bfloat16)
    across = (((1,), (1,)), ((), ()))
    d_hidden = lax.dot_general(rows_grad, w_down, across, preferred_element_type=jnp.float32)
    d_gate = (d_hidden * up * sig * (1.0 + gate * (1.0 - sig))).astype(jnp.bfloat16)
    d_up = (d_hidden * silu_gate).astype(jnp.bfloat16)
    grad_down = lax.dot_general(
        hidden, rows_grad, over_rows, preferred_element_type=jnp.float32
    ).astype(jnp.bfloat16)
    grad_gate = lax.dot_general(
        rows_input, d_gate, over_rows, preferred_element_type=jnp.float32
    ).astype(jnp.bfloat16)
    grad_up = lax.dot_general(
        rows_input, d_up, over_rows, preferred_element_type=jnp.float32
    ).astype(jnp.bfloat16)
    chunks = 2
    piece = capacity // chunks
    shape = (sp_devices, chunks, piece, d_gate.shape[1])
    gate_pieces = d_gate.reshape(shape)
    up_pieces = d_up.reshape(shape)
    shares = []
    for c in range(chunks):
        partial_input = lax.dot_general(
            gate_pieces[:, c].reshape(-1, shape[3]), w_gate, across,
            preferred_element_type=jnp.float32,
        ) + lax.dot_general(
            up_pieces[:, c].reshape(-1, shape[3]), w_up, across,
            preferred_element_type=jnp.float32,
        )
        shares.append(
            lax.psum_scatter(
                partial_input.astype(jnp.bfloat16), "tp", scatter_dimension=1, tiled=True
            )
        )
    shares[0], grad_down, grad_gate, grad_up = lax.optimization_barrier(
        (shares[0], grad_down, grad_gate, grad_up)
    )
    moe_grad = own_cotangent.astype(jnp.float32)
    pick_pieces = pick.reshape(experts, chunks, piece, tokens_here)
    for c in range(chunks):
        returned = to_owners(shares[c], sp_devices)
        moe_grad = moe_grad + lax.dot_general(
            pick_pieces[:, c].reshape(-1, tokens_here), returned, over_rows,
            preferred_element_type=jnp.float32,
        )
    stream_part = moe_grad.astype(jnp.bfloat16)
    stream_grad = lax.all_gather(stream_part, "tp", axis=1, tiled=True)
    own_projection = lax.dot_general(
        stream_grad, mixer_out, over_rows, preferred_element_type=jnp.float32
    ).astype(jnp.bfloat16)
    projections = to_owners(own_projection, sp_devices)
    grad_projection = jnp.sum(
        projections.astype(jnp.float32).reshape(sp_devices, -1, projections.shape[1]), axis=0
    )
    d_mixer = jnp.dot(stream_grad, out_proj, preferred_element_type=jnp.float32)
    grad_outer = d_mixer * conv_out
    d_conv = d_mixer * outer_gate.astype(jnp.float32)
    following = passed_along(d_conv[:2], "sp", -1)
    trailing = jnp.concatenate([d_conv, following], axis=0)
    d_mixed = (
        conv_taps[2] * trailing[:tokens_here]
        + conv_taps[1] * trailing[1 : tokens_here + 1]
        + conv_taps[0] * trailing[2:]
    )
    grad_inner = d_mixed * conv_input.astype(jnp.float32)
    grad_input = d_mixed * inner_gate.astype(jnp.float32)
    return (
        grad_gate[None],
        grad_up[None],
        grad_down[None],
        grad_projection,
        grad_outer,
        grad_inner,
        grad_input,
    )


def solution(mesh):
    placed = (
        P("sp", None),
        P("sp", None),
        P("sp", None),
        P("sp", None),
        P("sp", None, "tp"),
        P("sp", None, "tp"),
        P("sp", "tp", None),
        P("sp", "tp"),
        P("sp", "tp"),
        P("sp", "tp"),
        P(None, "tp"),
        P(None, "tp"),
    )
    return jax.shard_map(
        shards,
        mesh=mesh,
        in_specs=placed,
        out_specs=(
            P("sp", None, "tp"),
            P("sp", None, "tp"),
            P("sp", "tp", None),
            P("sp", "tp"),
            P("sp", "tp"),
            P("sp", "tp"),
            P("sp", "tp"),
        ),
        check_vma=False,
    )
```

```python
import jax
import jax.numpy as jnp
from jax import lax
from jax.sharding import PartitionSpec as P


def passed_along(x, axis, by):
    devices = lax.axis_size(axis)
    pairs = [(i, i + by) for i in range(devices) if 0 <= i + by < devices]
    return lax.ppermute(x, axis, pairs)


def to_owners(x, devices):
    blocks = x.reshape(devices, -1, x.shape[1])
    return lax.all_to_all(blocks, "sp", split_axis=0, concat_axis=0, tiled=True).reshape(x.shape)


def partial_rows(d_gate, d_up, w_gate, w_up):
    across = (((1,), (1,)), ((), ()))
    total = lax.dot_general(
        d_gate, w_gate, across, preferred_element_type=jnp.float32
    ) + lax.dot_general(d_up, w_up, across, preferred_element_type=jnp.float32)
    return total.astype(jnp.bfloat16)


def reduced_quarter(d_gate, d_up, w_gate, w_up):
    devices = lax.axis_size("tp")
    if devices != 4:
        return lax.psum_scatter(
            partial_rows(d_gate, d_up, w_gate, w_up), "tp", scatter_dimension=1, tiled=True
        )
    quarter = w_gate.shape[0] // devices
    me = lax.axis_index("tp")

    def rows_of(w, *flips):
        return jnp.concatenate(
            [lax.dynamic_slice_in_dim(w, (me ^ flip) * quarter, quarter, 0) for flip in flips]
        )

    def swapped(x, flip):
        return lax.ppermute(x, "tp", [(i, i ^ flip) for i in range(devices)])

    sent = partial_rows(d_gate, d_up, rows_of(w_gate, 1, 3), rows_of(w_up, 1, 3))
    got = swapped(sent, 1)
    kept = partial_rows(d_gate, d_up, rows_of(w_gate, 0, 2), rows_of(w_up, 0, 2))
    far = kept[:, quarter:].astype(jnp.float32) + got[:, quarter:].astype(jnp.float32)
    near = kept[:, :quarter].astype(jnp.float32) + got[:, :quarter].astype(jnp.float32)
    other = swapped(far.astype(jnp.bfloat16), 2)
    return (near + other.astype(jnp.float32)).astype(jnp.bfloat16)


def shards(
    out_cotangent,
    stream,
    route_ids,
    route_weights,
    gate_proj,
    up_proj,
    down_proj,
    outer_gate,
    inner_gate,
    conv_input,
    conv_taps,
    out_proj,
):
    sp_devices = lax.axis_size("sp")
    tokens_here, width = stream.shape
    experts = sp_devices * gate_proj.shape[0]
    capacity = 4 * tokens_here // experts
    quarter = width // lax.axis_size("tp")
    first_column = lax.axis_index("tp") * quarter
    own_cotangent = lax.dynamic_slice_in_dim(out_cotangent, first_column, quarter, 1)
    own_stream = lax.dynamic_slice_in_dim(stream, first_column, quarter, 1)
    over_rows = (((0,), (0,)), ((), ()))
    expert_ids = jnp.arange(experts, dtype=jnp.int32)
    chosen = route_ids[:, :, None] == expert_ids
    hit = jnp.any(chosen, axis=1)
    token_weight = jnp.sum(jnp.where(chosen, route_weights[:, :, None], 0.0), axis=1)
    token_ids = jnp.arange(tokens_here, dtype=jnp.int32)
    below = (token_ids[:, None] < token_ids[None, :]).astype(jnp.bfloat16)
    rank = lax.dot_general(
        hit.astype(jnp.bfloat16), below, over_rows, preferred_element_type=jnp.float32
    )
    rank = jnp.where(hit.T, rank, -1.0)
    in_slot = rank[:, None, :] == jnp.arange(capacity, dtype=jnp.float32)[None, :, None]
    slot_weight = jnp.sum(jnp.where(in_slot, token_weight.T[:, None, :], 0.0), axis=2)
    pick = in_slot.astype(jnp.bfloat16).reshape(experts * capacity, tokens_here)
    send_input = jnp.dot(pick, own_stream, preferred_element_type=jnp.float32).astype(jnp.bfloat16)
    send_grad = (
        slot_weight.reshape(-1, 1)
        * jnp.dot(pick, own_cotangent, preferred_element_type=jnp.float32)
    ).astype(jnp.bfloat16)
    got_input = to_owners(send_input, sp_devices)
    rows_input = lax.all_gather(got_input, "tp", axis=1, tiled=True)
    send_grad, got_input = lax.optimization_barrier((send_grad, got_input))
    got_grad = to_owners(send_grad, sp_devices)
    rows_grad = lax.all_gather(got_grad, "tp", axis=1, tiled=True)
    mixed = inner_gate.astype(jnp.float32) * conv_input.astype(jnp.float32)
    previous = passed_along(mixed[tokens_here - 2 :], "sp", 1)
    extended = jnp.concatenate([previous, mixed], axis=0)
    conv_out = (
        conv_taps[0] * extended[:tokens_here]
        + conv_taps[1] * extended[1 : tokens_here + 1]
        + conv_taps[2] * extended[2:]
    )
    mixer_out = (outer_gate.astype(jnp.float32) * conv_out).astype(jnp.bfloat16)
    conv_out, mixer_out, rows_grad = lax.optimization_barrier((conv_out, mixer_out, rows_grad))
    w_gate = gate_proj[0]
    w_up = up_proj[0]
    w_down = down_proj[0]
    gate = jnp.dot(rows_input, w_gate, preferred_element_type=jnp.float32)
    up = jnp.dot(rows_input, w_up, preferred_element_type=jnp.float32)
    sig = jax.nn.sigmoid(gate)
    silu_gate = gate * sig
    hidden = (silu_gate * up).astype(jnp.bfloat16)
    across = (((1,), (1,)), ((), ()))
    d_hidden = lax.dot_general(rows_grad, w_down, across, preferred_element_type=jnp.float32)
    d_gate = (d_hidden * up * sig * (1.0 + gate * (1.0 - sig))).astype(jnp.bfloat16)
    d_up = (d_hidden * silu_gate).astype(jnp.bfloat16)
    grad_down = lax.dot_general(
        hidden, rows_grad, over_rows, preferred_element_type=jnp.float32
    ).astype(jnp.bfloat16)
    grad_gate = lax.dot_general(
        rows_input, d_gate, over_rows, preferred_element_type=jnp.float32
    ).astype(jnp.bfloat16)
    grad_up = lax.dot_general(
        rows_input, d_up, over_rows, preferred_element_type=jnp.float32
    ).astype(jnp.bfloat16)
    chunks = 2
    piece = capacity // chunks
    shape = (sp_devices, chunks, piece, d_gate.shape[1])
    gate_pieces = d_gate.reshape(shape)
    up_pieces = d_up.reshape(shape)
    shares = []
    for c in range(chunks):
        shares.append(
            reduced_quarter(
                gate_pieces[:, c].reshape(-1, shape[3]),
                up_pieces[:, c].reshape(-1, shape[3]),
                w_gate,
                w_up,
            )
        )
    shares[0], grad_down, grad_gate, grad_up = lax.optimization_barrier(
        (shares[0], grad_down, grad_gate, grad_up)
    )
    moe_grad = own_cotangent.astype(jnp.float32)
    pick_pieces = pick.reshape(experts, chunks, piece, tokens_here)
    for c in range(chunks):
        returned = to_owners(shares[c], sp_devices)
        moe_grad = moe_grad + lax.dot_general(
            pick_pieces[:, c].reshape(-1, tokens_here), returned, over_rows,
            preferred_element_type=jnp.float32,
        )
    stream_part = moe_grad.astype(jnp.bfloat16)
    stream_grad = lax.all_gather(stream_part, "tp", axis=1, tiled=True)
    own_projection = lax.dot_general(
        stream_grad, mixer_out, over_rows, preferred_element_type=jnp.float32
    ).astype(jnp.bfloat16)
    projections = to_owners(own_projection, sp_devices)
    grad_projection = jnp.sum(
        projections.astype(jnp.float32).reshape(sp_devices, -1, projections.shape[1]), axis=0
    )
    d_mixer = jnp.dot(stream_grad, out_proj, preferred_element_type=jnp.float32)
    grad_outer = d_mixer * conv_out
    d_conv = d_mixer * outer_gate.astype(jnp.float32)
    following = passed_along(d_conv[:2], "sp", -1)
    trailing = jnp.concatenate([d_conv, following], axis=0)
    d_mixed = (
        conv_taps[2] * trailing[:tokens_here]
        + conv_taps[1] * trailing[1 : tokens_here + 1]
        + conv_taps[0] * trailing[2:]
    )
    grad_inner = d_mixed * conv_input.astype(jnp.float32)
    grad_input = d_mixed * inner_gate.astype(jnp.float32)
    return (
        grad_gate[None],
        grad_up[None],
        grad_down[None],
        grad_projection,
        grad_outer,
        grad_inner,
        grad_input,
    )


def solution(mesh):
    placed = (
        P("sp", None),
        P("sp", None),
        P("sp", None),
        P("sp", None),
        P("sp", None, "tp"),
        P("sp", None, "tp"),
        P("sp", "tp", None),
        P("sp", "tp"),
        P("sp", "tp"),
        P("sp", "tp"),
        P(None, "tp"),
        P(None, "tp"),
    )
    return jax.shard_map(
        shards,
        mesh=mesh,
        in_specs=placed,
        out_specs=(
            P("sp", None, "tp"),
            P("sp", None, "tp"),
            P("sp", "tp", None),
            P("sp", "tp"),
            P("sp", "tp"),
            P("sp", "tp"),
            P("sp", "tp"),
        ),
        check_vma=False,
    )
```

```python
import jax
import jax.numpy as jnp
from jax import lax
from jax.sharding import PartitionSpec as P


def passed_along(x, axis, by):
    devices = lax.axis_size(axis)
    pairs = [(i, i + by) for i in range(devices) if 0 <= i + by < devices]
    return lax.ppermute(x, axis, pairs)


def to_owners(x, devices):
    blocks = x.reshape(devices, -1, x.shape[1])
    return lax.all_to_all(blocks, "sp", split_axis=0, concat_axis=0, tiled=True).reshape(x.shape)


def partial_rows(d_gate, d_up, w_gate, w_up):
    across = (((1,), (1,)), ((), ()))
    total = lax.dot_general(
        d_gate, w_gate, across, preferred_element_type=jnp.float32
    ) + lax.dot_general(d_up, w_up, across, preferred_element_type=jnp.float32)
    return total.astype(jnp.bfloat16)


def reduced_quarter(d_gate, d_up, w_gate, w_up):
    devices = lax.axis_size("tp")
    if devices != 4:
        return lax.psum_scatter(
            partial_rows(d_gate, d_up, w_gate, w_up), "tp", scatter_dimension=1, tiled=True
        )
    quarter = w_gate.shape[0] // devices
    me = lax.axis_index("tp")

    def rows_of(w, *flips):
        return jnp.concatenate(
            [lax.dynamic_slice_in_dim(w, (me ^ flip) * quarter, quarter, 0) for flip in flips]
        )

    def swapped(x, flip):
        return lax.ppermute(x, "tp", [(i, i ^ flip) for i in range(devices)])

    sent = partial_rows(d_gate, d_up, rows_of(w_gate, 1, 3), rows_of(w_up, 1, 3))
    got = swapped(sent, 1)
    kept = partial_rows(d_gate, d_up, rows_of(w_gate, 0, 2), rows_of(w_up, 0, 2))
    far = kept[:, quarter:].astype(jnp.float32) + got[:, quarter:].astype(jnp.float32)
    near = kept[:, :quarter].astype(jnp.float32) + got[:, :quarter].astype(jnp.float32)
    other = swapped(far.astype(jnp.bfloat16), 2)
    return (near + other.astype(jnp.float32)).astype(jnp.bfloat16)


def shards(
    out_cotangent,
    stream,
    route_ids,
    route_weights,
    gate_proj,
    up_proj,
    down_proj,
    outer_gate,
    inner_gate,
    conv_input,
    conv_taps,
    out_proj,
):
    sp_devices = lax.axis_size("sp")
    tokens_here, width = stream.shape
    experts = sp_devices * gate_proj.shape[0]
    capacity = 4 * tokens_here // experts
    quarter = width // lax.axis_size("tp")
    first_column = lax.axis_index("tp") * quarter
    own_cotangent = lax.dynamic_slice_in_dim(out_cotangent, first_column, quarter, 1)
    own_stream = lax.dynamic_slice_in_dim(stream, first_column, quarter, 1)
    over_rows = (((0,), (0,)), ((), ()))
    expert_ids = jnp.arange(experts, dtype=jnp.int32)
    chosen = route_ids[:, :, None] == expert_ids
    hit = jnp.any(chosen, axis=1)
    token_weight = jnp.sum(jnp.where(chosen, route_weights[:, :, None], 0.0), axis=1)
    token_ids = jnp.arange(tokens_here, dtype=jnp.int32)
    below = (token_ids[:, None] < token_ids[None, :]).astype(jnp.bfloat16)
    rank = lax.dot_general(
        hit.astype(jnp.bfloat16), below, over_rows, preferred_element_type=jnp.float32
    )
    rank = jnp.where(hit.T, rank, -1.0)
    chunks = 2
    piece = capacity // chunks
    picks, inputs, grads = [], [], []
    last = None
    for c in range(chunks):
        slots = jnp.arange(c * piece, (c + 1) * piece, dtype=jnp.int32).astype(jnp.float32)
        in_slot = rank[:, None, :] == slots[None, :, None]
        slot_weight = jnp.sum(jnp.where(in_slot, token_weight.T[:, None, :], 0.0), axis=2)
        pick = in_slot.astype(jnp.bfloat16).reshape(experts * piece, tokens_here)
        send_input = jnp.dot(pick, own_stream, preferred_element_type=jnp.float32)
        send_grad = slot_weight.reshape(-1, 1) * jnp.dot(
            pick, own_cotangent, preferred_element_type=jnp.float32
        )
        picks.append(pick)
        for rows, send in ((inputs, send_input), (grads, send_grad)):
            send = send.astype(jnp.bfloat16)
            if last is not None:
                send, last = lax.optimization_barrier((send, last))
            last = to_owners(send, sp_devices)
            rows.append(lax.all_gather(last, "tp", axis=1, tiled=True))
    mixed = inner_gate.astype(jnp.float32) * conv_input.astype(jnp.float32)
    previous = passed_along(mixed[tokens_here - 2 :], "sp", 1)
    extended = jnp.concatenate([previous, mixed], axis=0)
    conv_out = (
        conv_taps[0] * extended[:tokens_here]
        + conv_taps[1] * extended[1 : tokens_here + 1]
        + conv_taps[2] * extended[2:]
    )
    mixer_out = (outer_gate.astype(jnp.float32) * conv_out).astype(jnp.bfloat16)
    conv_out, mixer_out, grads[0] = lax.optimization_barrier((conv_out, mixer_out, grads[0]))
    w_gate = gate_proj[0]
    w_up = up_proj[0]
    w_down = down_proj[0]
    across = (((1,), (1,)), ((), ()))
    shares = []
    grad_down = grad_gate = grad_up = 0.0
    for rows_input, rows_grad in zip(inputs, grads):
        gate = jnp.dot(rows_input, w_gate, preferred_element_type=jnp.float32)
        up = jnp.dot(rows_input, w_up, preferred_element_type=jnp.float32)
        sig = jax.nn.sigmoid(gate)
        silu_gate = gate * sig
        hidden = (silu_gate * up).astype(jnp.bfloat16)
        d_hidden = lax.dot_general(rows_grad, w_down, across, preferred_element_type=jnp.float32)
        d_gate = (d_hidden * up * sig * (1.0 + gate * (1.0 - sig))).astype(jnp.bfloat16)
        d_up = (d_hidden * silu_gate).astype(jnp.bfloat16)
        shares.append(reduced_quarter(d_gate, d_up, w_gate, w_up))
        grad_down += lax.dot_general(
            hidden, rows_grad, over_rows, preferred_element_type=jnp.float32
        )
        grad_gate += lax.dot_general(
            rows_input, d_gate, over_rows, preferred_element_type=jnp.float32
        )
        grad_up += lax.dot_general(
            rows_input, d_up, over_rows, preferred_element_type=jnp.float32
        )
    grad_down = grad_down.astype(jnp.bfloat16)
    grad_gate = grad_gate.astype(jnp.bfloat16)
    grad_up = grad_up.astype(jnp.bfloat16)
    shares[-1], grad_down, grad_gate, grad_up = lax.optimization_barrier(
        (shares[-1], grad_down, grad_gate, grad_up)
    )
    moe_grad = own_cotangent.astype(jnp.float32)
    for c in range(chunks):
        returned = to_owners(shares[c], sp_devices)
        moe_grad = moe_grad + lax.dot_general(
            picks[c], returned, over_rows,
            preferred_element_type=jnp.float32,
        )
    stream_part = moe_grad.astype(jnp.bfloat16)
    stream_grad = lax.all_gather(stream_part, "tp", axis=1, tiled=True)
    own_projection = lax.dot_general(
        stream_grad, mixer_out, over_rows, preferred_element_type=jnp.float32
    ).astype(jnp.bfloat16)
    projections = to_owners(own_projection, sp_devices)
    grad_projection = jnp.sum(
        projections.astype(jnp.float32).reshape(sp_devices, -1, projections.shape[1]), axis=0
    )
    d_mixer = jnp.dot(stream_grad, out_proj, preferred_element_type=jnp.float32)
    grad_outer = d_mixer * conv_out
    d_conv = d_mixer * outer_gate.astype(jnp.float32)
    following = passed_along(d_conv[:2], "sp", -1)
    trailing = jnp.concatenate([d_conv, following], axis=0)
    d_mixed = (
        conv_taps[2] * trailing[:tokens_here]
        + conv_taps[1] * trailing[1 : tokens_here + 1]
        + conv_taps[0] * trailing[2:]
    )
    grad_inner = d_mixed * conv_input.astype(jnp.float32)
    grad_input = d_mixed * inner_gate.astype(jnp.float32)
    return (
        grad_gate[None],
        grad_up[None],
        grad_down[None],
        grad_projection,
        grad_outer,
        grad_inner,
        grad_input,
    )


def solution(mesh):
    placed = (
        P("sp", None),
        P("sp", None),
        P("sp", None),
        P("sp", None),
        P("sp", None, "tp"),
        P("sp", None, "tp"),
        P("sp", "tp", None),
        P("sp", "tp"),
        P("sp", "tp"),
        P("sp", "tp"),
        P(None, "tp"),
        P(None, "tp"),
    )
    return jax.shard_map(
        shards,
        mesh=mesh,
        in_specs=placed,
        out_specs=(
            P("sp", None, "tp"),
            P("sp", None, "tp"),
            P("sp", "tp", None),
            P("sp", "tp"),
            P("sp", "tp"),
            P("sp", "tp"),
            P("sp", "tp"),
        ),
        check_vma=False,
    )
```
